32 devices in a mesh: sp: 8 (over z, x), tp: 4 (over y, core).
Axes of the slice: x: 2, y: 2, z: 4, core: 2. Of those that a mesh axis runs over, the one named last changes fastest.
Arguments:
- tokens: bfloat16 [2048, 2048], P(('sp', 'tp')), may hold values from -40 to 40
- w_query: bfloat16 [2048, 1024], P(None, 'tp'), may hold values from -0.125 to 0.125
- w_key: bfloat16 [2048, 256], P(None, 'tp'), may hold values from -0.125 to 0.125
- w_value: bfloat16 [2048, 256], P(None, 'tp'), may hold values from -0.125 to 0.125
- w_out: bfloat16 [1024, 2048], P('tp'), may hold values from -0.1875 to 0.1875
- cum_gate: float32 [16, 2048], P('tp', 'sp'), may hold values from -295 to 0, as said below
Outputs:
- layer_out: bfloat16 [2048, 2048], P(('sp', 'tp'))
The draws below stay inside these ranges and needn't reach their ends.
Inputs may be any that keep to these rules, and one draw needn't show every extreme that they name: `cum_gate`: each head's row does not rise along the positions.
All inputs are finite; a program needn't handle non-finite values.
Results may differ from the reference program's by a relative error of at most 0.012.
Values may be sent and summed in bfloat16 or wider, within the bound.
A program may use at most 64 MiB of HBM per device.

```python
import math
import jax
import jax.numpy as jnp
from jax import lax

D = 2048
H = 16
KVH = 4
HD = 64
TOK_DEV = 256
STREAM_LENGTH = 2048


def draw_tokens(key, part):
    keys = jax.random.split(key, 3)
    base = jnp.clip(jax.random.normal(keys[0], (STREAM_LENGTH, D), jnp.float32), -6.0, 6.0)
    direction = jnp.clip(jax.random.normal(keys[1], (D,), jnp.float32), -4.0, 4.0)
    level = jax.random.uniform(keys[2], (STREAM_LENGTH // TOK_DEV,), jnp.float32, -1.5, 1.5)
    shifted = jnp.repeat(level, TOK_DEV)
    result = base + shifted[:, None] * direction[None, :]
    return result.astype(jnp.bfloat16)


def draw_cum_gate(key, part):
    keys = jax.random.split(key, 6)
    order = jax.random.permutation(keys[0], H)
    gentle_fading_rate = order < H // 2
    whole_loss = jnp.exp(jax.random.uniform(keys[1], (H,), jnp.float32, math.log(0.3), math.log(1.0)))
    slow_rate = whole_loss / STREAM_LENGTH
    fast_rate = jnp.exp(jax.random.uniform(keys[2], (H,), jnp.float32, math.log(0.01), math.log(1.0 / 30.0)))
    rate = jnp.where(gentle_fading_rate, slow_rate, fast_rate)
    device_multiplier = jnp.exp(jax.random.uniform(keys[3], (STREAM_LENGTH // TOK_DEV,), jnp.float32, math.log(0.5), math.log(2.0)))
    factor_tokens = jnp.repeat(device_multiplier, TOK_DEV)
    rough = jax.random.uniform(keys[4], (H, STREAM_LENGTH), jnp.float32, 0.0, 2.0)
    log_forget_factor = -rate[:, None] * factor_tokens[None, :] * rough
    probe_indices = jax.random.randint(keys[5], (3,), 0, STREAM_LENGTH)
    objective_terms = jax.random.uniform(jax.random.fold_in(key, 9), (3,), jnp.float32, math.log(0.5), math.log(0.8))
    key_head_clusters = jnp.zeros((STREAM_LENGTH,), jnp.float32).at[probe_indices].add(objective_terms)
    log_forget_factor = log_forget_factor + jnp.where(gentle_fading_rate[:, None], key_head_clusters[None, :], 0.0)
    return jnp.cumsum(log_forget_factor, axis=1)


def level_of(rng, dims, cuts, low, largest):
    def one(position, blocks):
        heights = jax.random.uniform(jax.random.fold_in(jax.random.fold_in(rng, 6), position), (blocks,), jnp.float32, low / len(cuts), largest / len(cuts))
        return jnp.repeat(jnp.exp(heights), dims[position] // blocks).reshape((-1,) + (1,) * (len(dims) - position - 1))

    gain = one(*cuts[0])
    for cut in cuts[1:]:
        gain = gain * one(*cut)
    return gain


def scatter_about(key, extent, deviation, bound, cuts=(), kind=jnp.bfloat16):
    values = deviation * jax.random.normal(key, extent, jnp.float32)
    if cuts:
        values = values * level_of(key, extent, cuts, -0.22, 0.18)
    return jnp.clip(values, -bound, bound).astype(kind)


def setup_inputs(seed: int = 0) -> dict:
    key_of = jax.random.split(jax.random.key(seed), 7)
    tokens = draw_tokens(jax.random.fold_in(key_of[6], 71), 0)
    w_query = scatter_about(key_of[1], (D, H * HD), D ** -0.5, 0.125, ((1, 4),))
    w_key = scatter_about(key_of[2], (D, KVH * HD), D ** -0.5, 0.125, ((1, 4),))
    w_value = scatter_about(key_of[3], (D, KVH * HD), D ** -0.5, 0.125, ((1, 4),))
    w_out = scatter_about(key_of[4], (H * HD, D), (H * HD) ** -0.5, 0.1875, ((0, 4),))
    cum_gate = draw_cum_gate(jax.random.fold_in(key_of[6], 71), 0)
    return dict(tokens=tokens, w_query=w_query, w_key=w_key, w_value=w_value, w_out=w_out, cum_gate=cum_gate)


def reference(tokens, w_query, w_key, w_value, w_out, cum_gate):
    length_all = tokens.shape[0]
    queries = jnp.dot(tokens, w_query, preferred_element_type=jnp.float32).astype(jnp.bfloat16)
    key_proj = jnp.dot(tokens, w_key, preferred_element_type=jnp.float32).astype(jnp.bfloat16)
    values = jnp.dot(tokens, w_value, preferred_element_type=jnp.float32).astype(jnp.bfloat16)
    group_size = H // KVH
    block_rows = math.gcd(length_all, 256)
    block_count = length_all // block_rows
    score_factor = float(HD) ** -0.5
    keys_wide = key_proj.astype(jnp.float32).reshape(length_all, KVH, HD)
    values_wide = values.astype(jnp.float32).reshape(length_all, KVH, HD)
    cum_keys = cum_gate.reshape(KVH, group_size, length_all)
    query_blocks = queries.reshape(block_count, block_rows, KVH, group_size, HD)
    cum_blocks = cum_gate.reshape(KVH, group_size, block_count, block_rows).transpose(2, 0, 1, 3)
    starts = jnp.arange(block_count, dtype=jnp.int32) * block_rows
    key_pos = jnp.arange(length_all, dtype=jnp.int32)

    def attend(bundle):
        query_block, cum_block, offset = bundle
        scores = jnp.einsum('tkgd,skd->kgts', query_block.astype(jnp.float32), keys_wide) * score_factor
        scores = scores + (cum_block[..., None] - cum_keys[:, :, None, :])
        query_pos = offset + jnp.arange(block_rows, dtype=jnp.int32)
        scores = jnp.where(key_pos[None, :] <= query_pos[:, None], scores, -jnp.inf)
        row_max = jnp.max(scores, axis=-1, keepdims=True)
        weights = jnp.exp(scores - row_max)
        totals = jnp.sum(weights, axis=-1)
        rounded = lax.optimization_barrier(weights.astype(jnp.bfloat16)).astype(jnp.float32)
        attended = jnp.einsum('kgts,skd->kgtd', rounded, values_wide) / totals[..., None]
        return attended.astype(jnp.bfloat16).transpose(2, 0, 1, 3).reshape(block_rows, H * HD)

    attended = lax.map(attend, (query_blocks, cum_blocks, starts)).reshape(length_all, H * HD)
    return jnp.dot(attended, w_out, preferred_element_type=jnp.float32).astype(jnp.bfloat16)
```

```python
import functools

import jax
import jax.numpy as jnp
from jax import lax
from jax.experimental import pallas as pl
from jax.experimental.pallas import tpu as pltpu
from jax.sharding import PartitionSpec as P

HD = 64
MESH = pl.DeviceIdType.MESH
CHUNKS = 4


def kernel(
    sp_size, tok, wq, wk, wv, wo, gate, out,
    x, wqv, wkv, wvv, wov, gv, kv, qt, top, tot, acc, att, pf, own,
    s_near, s_far, s_own, r_near, r_far, r_own,
    load, tok_s, tok_r, far_s, far_r, fwd_s, fwd_r,
    z_s, x_s, kv_r, o_s, o_r,
):
    f32, bf16 = jnp.float32, jnp.bfloat16
    rows = tok.shape[0]
    half = 2 * rows
    block = 2 * half
    heads = wq.shape[1] // HD
    sp = lax.axis_index("sp")
    t = lax.axis_index("tp")
    core = lax.rem(t, 2)
    p = t // 2
    t1 = t + 1 - 2 * core
    t2 = lax.rem(t + 2, 4)
    r = sp // 2
    c = lax.rem(sp, 2)
    last_row = sp_size // 2 - 1
    spx = sp + 1 - 2 * c
    has_next = r < last_row
    pa, pb = p, 1 - p

    def at(n, unit):
        return pl.ds(pl.multiple_of(n * unit, unit), unit)

    loads = [
        pltpu.make_async_copy(tok, x.at[at(t, rows)], load.at[0]),
        pltpu.make_async_copy(gate, gv, load.at[1]),
        pltpu.make_async_copy(wk, wkv, load.at[2]),
        pltpu.make_async_copy(wv, wvv, load.at[3]),
        pltpu.make_async_copy(wq, wqv, load.at[4]),
        pltpu.make_async_copy(wo, wov, load.at[5]),
    ]
    for copy in loads:
        copy.start()

    barrier = pltpu.get_barrier_semaphore()
    pl.semaphore_signal(barrier, inc=1, device_id={"tp": t1}, device_id_type=MESH)
    pl.semaphore_signal(barrier, inc=1, device_id={"tp": t2}, device_id_type=MESH)
    pl.semaphore_signal(barrier, inc=1, device_id={"sp": spx}, device_id_type=MESH)

    @pl.when(has_next)
    def _():
        pl.semaphore_signal(barrier, inc=1, device_id={"sp": sp + 2}, device_id_type=MESH)

    @pl.when(r > 0)
    def _():
        pl.semaphore_signal(barrier, inc=1, device_id={"sp": sp - 2}, device_id_type=MESH)

    peers = 3 + jnp.where(has_next, 1, 0) + jnp.where(r > 0, 1, 0)
    pl.semaphore_wait(barrier, peers)

    step = rows // CHUNKS

    def piece(shard, n):
        return pl.ds(pl.multiple_of(shard * rows + n * step, step), step)

    def remote(src, dst, ss, rs, **where):
        return pltpu.make_async_remote_copy(
            src_ref=src, dst_ref=dst, send_sem=ss, recv_sem=rs,
            device_id=where, device_id_type=MESH,
        )

    far = []
    for n in range(CHUNKS):
        cp = remote(tok.at[pl.ds(n * step, step)], x.at[piece(t, n)], far_s.at[n], far_r.at[n], tp=t2)
        cp.start()
        far.append(cp)
    near = remote(tok, x.at[at(t, rows)], tok_s.at[0], tok_r.at[0], tp=t1)
    near.start()

    loads[1].wait()
    g = gv[...]
    hi = g.astype(bf16).astype(f32)
    mid = (g - hi).astype(bf16).astype(f32)
    low = (g - hi - mid).astype(bf16).astype(f32)
    parts = (hi, mid, low)
    extra = kv.shape[2] - 2 * HD
    index = lax.broadcasted_iota(jnp.int32, (extra, block), 0)
    key_side = jnp.where((index >= 3 * heads) & (index < 3 * heads + 3), 1.0, 0.0).astype(f32)
    for k in range(3):
        for h in range(heads):
            key_side = jnp.where(index == k * heads + h, -parts[k][h : h + 1, :], key_side)
    key_side = key_side.astype(bf16)
    kv[sp, 0, HD : HD + extra, :] = key_side[:, :half]
    kv[sp, 1, HD : HD + extra, :] = key_side[:, half:]
    for h in range(heads):
        side = jnp.where((index < 3 * heads) & (lax.rem(index, heads) == h), 1.0, 0.0).astype(f32)
        for k in range(3):
            side = jnp.where(index == 3 * heads + k, parts[k][h : h + 1, :], side)
        qt[h, HD : HD + extra, :] = side.astype(bf16)

    def project_kv(which):
        xs = x[at(which, half), :]
        key = jnp.dot(xs, wkv[...], preferred_element_type=f32)
        val = jnp.dot(xs, wvv[...], preferred_element_type=f32)
        both = jnp.concatenate([key, val], axis=1).T.astype(bf16)
        kv[sp, which, 0:HD, :] = both[:HD]
        kv[sp, which, HD + extra :, :] = both[HD:]

    def project_q(which):
        xs = x[at(which, half), :]
        q = jnp.dot(xs, wqv[...], preferred_element_type=f32).astype(bf16).astype(f32)
        q = (q * (float(HD) ** -0.5)).T.astype(bf16)
        for h in range(heads):
            qt[h, 0:HD, at(which, half)] = q[h * HD : (h + 1) * HD]

    def along(src, which):
        ref = kv.at[src, which]
        return remote(ref, ref, z_s.at[src // 2, which], kv_r.at[src, which], sp=sp + 2)

    def across(src, which):
        ref = kv.at[src, which]
        return remote(ref, ref, x_s.at[src // 2, which], kv_r.at[src, which], sp=spx)

    def send_own(which):
        @pl.when(has_next)
        def _():
            along(sp, which).start()

        @pl.when(c == 0)
        def _():
            across(sp, which).start()

    def relay(i, which):
        src = sp - 2 * i
        along(src, which).wait_recv()

        @pl.when(has_next)
        def _():
            along(src, which).start()

        across(src, which).start()

    loads[0].wait()
    loads[2].wait()
    loads[3].wait()
    near.wait_recv()
    project_kv(pa)
    send_own(pa)
    loads[4].wait()
    project_q(pa)

    fwd = []
    for n in range(CHUNKS):
        far[n].wait_recv()
        ref = x.at[piece(t2, n)]
        cp = remote(ref, ref, fwd_s.at[n], fwd_r.at[n], tp=t1)
        cp.start()
        fwd.append(cp)

        @pl.when(r >= n + 1)
        def _(n=n):
            relay(n + 1, pa)

    @pl.loop(CHUNKS + 1, r + 1)
    def _(i):
        relay(i, pa)

    for n in range(CHUNKS):
        fwd[n].wait_recv()
    project_kv(pb)
    send_own(pb)
    project_q(pb)

    def attend(src, diagonal):
        kt = jnp.concatenate([kv[src, 0, 0 : HD + extra, :], kv[src, 1, 0 : HD + extra, :]], axis=1)
        vt = jnp.concatenate([kv[src, 0, HD + extra :, :], kv[src, 1, HD + extra :, :]], axis=1)
        for h in range(heads):
            s = lax.dot_general(kt, qt[h], (((0,), (0,)), ((), ())), preferred_element_type=f32)
            lanes = slice(h * HD, (h + 1) * HD)
            if diagonal:
                key_pos = lax.broadcasted_iota(jnp.int32, s.shape, 0)
                query_pos = lax.broadcasted_iota(jnp.int32, s.shape, 1)
                s = jnp.where(key_pos <= query_pos, s, -jnp.inf)
                peak = jnp.max(s, axis=0, keepdims=True)
                w = jnp.exp(s - peak)
                tot[h : h + 1, :] = jnp.sum(w, axis=0, keepdims=True)
                acc[lanes, :] = jnp.dot(vt, w.astype(bf16), preferred_element_type=f32)
            else:
                before = top[h : h + 1, :]
                peak = jnp.maximum(before, jnp.max(s, axis=0, keepdims=True))
                w = jnp.exp(s - peak)
                decay = jnp.exp(before - peak)
                tot[h : h + 1, :] = tot[h : h + 1, :] * decay + jnp.sum(w, axis=0, keepdims=True)
                acc[lanes, :] = acc[lanes, :] * decay + jnp.dot(
                    vt, w.astype(bf16), preferred_element_type=f32
                )
            top[h : h + 1, :] = peak

    attend(sp, True)

    def wait_across(src):
        for which in (pa, pb):
            across(src, which).wait_recv()

    @pl.when(c == 1)
    def _():
        wait_across(spx)
        attend(spx, False)

    @pl.loop(1, r + 1)
    def _(i):
        relay(i, pb)
        attend(sp - 2 * i, False)
        wait_across(spx - 2 * i)
        attend(spx - 2 * i, False)

    for h in range(heads):
        lanes = slice(h * HD, (h + 1) * HD)
        acc[lanes, :] = acc[lanes, :] / tot[h : h + 1, :]
    att[...] = acc[...].T.astype(bf16)
    loads[5].wait()
    width = wo.shape[1] // CHUNKS
    near_sum, far_sum, own_sum = [], [], []
    for n in range(CHUNKS):
        cols = slice(n * width, (n + 1) * width)
        pf[:, cols] = jnp.dot(att[at(pb, half), :], wov[:, cols], preferred_element_type=f32)
        s_near[n] = pf[at(1 - core, rows), cols].astype(bf16)
        cp = remote(s_near.at[n], r_near.at[n], o_s.at[0, n], o_r.at[0, n], tp=t1)
        cp.start()
        near_sum.append(cp)
    for n in range(CHUNKS):
        cols = slice(n * width, (n + 1) * width)
        near_sum[n].wait_recv()
        s_far[n] = (pf[at(core, rows), cols] + r_near[n].astype(f32)).astype(bf16)
        cp = remote(s_far.at[n], r_far.at[n], o_s.at[1, n], o_r.at[1, n], tp=t2)
        cp.start()
        far_sum.append(cp)
    for n in range(CHUNKS):
        cols = slice(n * width, (n + 1) * width)
        own[:, cols] = jnp.dot(att[at(pa, half), :], wov[:, cols], preferred_element_type=f32)
        s_own[n] = own[at(1 - core, rows), cols].astype(bf16)
        cp = remote(s_own.at[n], r_own.at[n], o_s.at[2, n], o_r.at[2, n], tp=t1)
        cp.start()
        own_sum.append(cp)
    for n in range(CHUNKS):
        cols = slice(n * width, (n + 1) * width)
        own_sum[n].wait_recv()
        far_sum[n].wait_recv()
        total = own[at(core, rows), cols] + r_own[n].astype(f32) + r_far[n].astype(f32)
        out[:, cols] = total.astype(bf16)

    near.wait_send()
    for cp in far + fwd + near_sum + far_sum + own_sum:
        cp.wait_send()
    for which in (pa, pb):

        @pl.when(c == 0)
        def _(which=which):
            across(sp, which).wait_send()

        @pl.when(has_next)
        def _(which=which):
            along(sp, which).wait_send()

            @pl.loop(1, r + 1)
            def _(i):
                along(sp - 2 * i, which).wait_send()

        @pl.loop(1, r + 1)
        def _(i, which=which):
            across(sp - 2 * i, which).wait_send()


def per_device(sp_size, tokens, w_query, w_key, w_value, w_out, cum_gate):
    rows, width = tokens.shape
    half, block = 2 * rows, 4 * rows
    heads = w_query.shape[1] // HD
    out_width = w_out.shape[1]
    extra = -(-(3 * heads + 3) // 16) * 16
    bf16, f32 = jnp.bfloat16, jnp.float32
    dma = pltpu.SemaphoreType.DMA
    anywhere = pl.BlockSpec(memory_space=pl.ANY)
    part = pltpu.VMEM((CHUNKS, rows, out_width // CHUNKS), bf16)
    return pl.pallas_call(
        functools.partial(kernel, sp_size),
        out_shape=jax.ShapeDtypeStruct((rows, out_width), bf16),
        in_specs=[anywhere] * 6,
        out_specs=pl.BlockSpec(memory_space=pltpu.VMEM),
        scratch_shapes=[
            pltpu.VMEM((block, width), bf16),
            pltpu.VMEM(w_query.shape, bf16),
            pltpu.VMEM(w_key.shape, bf16),
            pltpu.VMEM(w_value.shape, bf16),
            pltpu.VMEM(w_out.shape, bf16),
            pltpu.VMEM(cum_gate.shape, f32),
            pltpu.VMEM((sp_size, 2, 2 * HD + extra, half), bf16),
            pltpu.VMEM((heads, HD + extra, block), bf16),
            pltpu.VMEM((heads, block), f32),
            pltpu.VMEM((heads, block), f32),
            pltpu.VMEM((heads * HD, block), f32),
            pltpu.VMEM((block, heads * HD), bf16),
            pltpu.VMEM((half, out_width), f32),
            pltpu.VMEM((half, out_width), f32),
            part, part, part, part, part, part,
            dma((6,)),
            dma((1,)), dma((1,)),
            dma((CHUNKS,)), dma((CHUNKS,)),
            dma((CHUNKS,)), dma((CHUNKS,)),
            dma((sp_size // 2, 2)), dma((sp_size // 2, 2)), dma((sp_size, 2)),
            dma((3, CHUNKS)), dma((3, CHUNKS)),
        ],
        compiler_params=pltpu.CompilerParams(
            collective_id=0, has_side_effects=True, vmem_limit_bytes=48 * 1024 * 1024
        ),
    )(tokens, w_query, w_key, w_value, w_out, cum_gate)


def solution(mesh):
    placed = (
        P(("sp", "tp"), None),
        P(None, "tp"),
        P(None, "tp"),
        P(None, "tp"),
        P("tp", None),
        P("tp", "sp"),
    )
    return jax.shard_map(
        functools.partial(per_device, mesh.shape["sp"]),
        mesh=mesh, in_specs=placed, out_specs=P(("sp", "tp"), None), check_vma=False,
    )
```

```python
import functools

import jax
import jax.numpy as jnp
from jax import lax
from jax.experimental import pallas as pl
from jax.experimental.pallas import tpu as pltpu
from jax.sharding import PartitionSpec as P

HD = 64
MESH = pl.DeviceIdType.MESH
CHUNKS = 4


def kernel(
    sp_size, tok, wq, wk, wv, wo, gate, out,
    x, wqv, wkv, wvv, wboth, wov, gv, kv, qt, top, tot, acc, att, pf, own,
    s_near, s_far, s_own, r_near, r_far, r_own,
    load, tok_s, tok_r, far_s, far_r, fwd_s, fwd_r,
    z_s, x_s, kv_r, o_s, o_r, ready,
):
    f32, bf16 = jnp.float32, jnp.bfloat16
    rows = tok.shape[0]
    half = 2 * rows
    block = 2 * half
    heads = wq.shape[1] // HD
    sp = lax.axis_index("sp")
    t = lax.axis_index("tp")
    core = lax.rem(t, 2)
    p = t // 2
    t1 = t + 1 - 2 * core
    t2 = lax.rem(t + 2, 4)
    r = sp // 2
    c = lax.rem(sp, 2)
    last_row = sp_size // 2 - 1
    spx = sp + 1 - 2 * c
    has_next = r < last_row
    pa, pb = p, 1 - p

    def at(n, unit):
        return pl.ds(pl.multiple_of(n * unit, unit), unit)

    loads = [
        pltpu.make_async_copy(tok, x.at[at(t, rows)], load.at[0]),
        pltpu.make_async_copy(gate, gv, load.at[1]),
        pltpu.make_async_copy(wk, wkv, load.at[2]),
        pltpu.make_async_copy(wv, wvv, load.at[3]),
        pltpu.make_async_copy(wq, wqv, load.at[4]),
        pltpu.make_async_copy(wo, wov, load.at[5]),
    ]
    for copy in loads:
        copy.start()

    barrier = pltpu.get_barrier_semaphore()
    pl.semaphore_signal(barrier, inc=1, device_id={"tp": t1}, device_id_type=MESH)
    pl.semaphore_signal(barrier, inc=1, device_id={"tp": t2}, device_id_type=MESH)
    pl.semaphore_signal(barrier, inc=1, device_id={"sp": spx}, device_id_type=MESH)

    @pl.when(has_next)
    def _():
        pl.semaphore_signal(barrier, inc=1, device_id={"sp": sp + 2}, device_id_type=MESH)

    @pl.when(r > 0)
    def _():
        pl.semaphore_signal(barrier, inc=1, device_id={"sp": sp - 2}, device_id_type=MESH)

    peers = 3 + jnp.where(has_next, 1, 0) + jnp.where(r > 0, 1, 0)
    pl.semaphore_wait(barrier, peers)

    step = rows // CHUNKS

    def piece(shard, n):
        return pl.ds(pl.multiple_of(shard * rows + n * step, step), step)

    def remote(src, dst, ss, rs, **where):
        return pltpu.make_async_remote_copy(
            src_ref=src, dst_ref=dst, send_sem=ss, recv_sem=rs,
            device_id=where, device_id_type=MESH,
        )

    far = []
    for n in range(CHUNKS):
        cp = remote(tok.at[pl.ds(n * step, step)], x.at[piece(t, n)], far_s.at[n], far_r.at[n], tp=t2)
        cp.start()
        far.append(cp)
    near = remote(tok, x.at[at(t, rows)], tok_s.at[0], tok_r.at[0], tp=t1)
    near.start()

    @pl.when(has_next)
    def _():
        pl.semaphore_wait(ready, 1)

    @pl.when(r > 0)
    def _():
        pl.semaphore_signal(ready, inc=1, device_id={"sp": sp - 2}, device_id_type=MESH)

    loads[2].wait()
    loads[3].wait()
    wboth[...] = jnp.concatenate([wkv[...], wvv[...]], axis=1)

    loads[1].wait()
    g = gv[...]
    hi = g.astype(bf16).astype(f32)
    mid = (g - hi).astype(bf16).astype(f32)
    low = (g - hi - mid).astype(bf16).astype(f32)
    parts = (hi, mid, low)
    extra = kv.shape[2] - 2 * HD
    index = lax.broadcasted_iota(jnp.int32, (extra, block), 0)
    key_side = jnp.where((index >= 3 * heads) & (index < 3 * heads + 3), 1.0, 0.0).astype(f32)
    for k in range(3):
        for h in range(heads):
            key_side = jnp.where(index == k * heads + h, -parts[k][h : h + 1, :], key_side)
    key_side = key_side.astype(bf16)
    kv[sp, 0, HD : HD + extra, :] = key_side[:, :half]
    kv[sp, 1, HD : HD + extra, :] = key_side[:, half:]
    for h in range(heads):
        side = jnp.where((index < 3 * heads) & (lax.rem(index, heads) == h), 1.0, 0.0).astype(f32)
        for k in range(3):
            side = jnp.where(index == 3 * heads + k, parts[k][h : h + 1, :], side)
        qt[h, HD : HD + extra, :] = side.astype(bf16)

    def project_kv(which):
        xs = x[at(which, half), :]
        both = jnp.dot(xs, wboth[...], preferred_element_type=f32).T.astype(bf16)
        kv[sp, which, 0:HD, :] = both[:HD]
        kv[sp, which, HD + extra :, :] = both[HD:]

    def project_q(which):
        xs = x[at(which, half), :]
        q = jnp.dot(xs, wqv[...], preferred_element_type=f32).astype(bf16).astype(f32)
        q = (q * (float(HD) ** -0.5)).T.astype(bf16)
        for h in range(heads):
            qt[h, 0:HD, at(which, half)] = q[h * HD : (h + 1) * HD]

    def along(src, which, row):
        ref = kv.at[src, which]
        return remote(ref, ref, z_s.at[row, which], kv_r.at[src, which], sp=2 * row + c)

    def across(src, which):
        ref = kv.at[src, which]
        return remote(ref, ref, x_s.at[src // 2, which], kv_r.at[src, which], sp=spx)

    def send_own(which):
        @pl.loop(0, last_row - r)
        def _(i):
            along(sp, which, last_row - i).start()

        @pl.when(c == 0)
        def _():
            across(sp, which).start()

    def relay(which):
        @pl.loop(1, r + 1)
        def _(i):
            across(sp - 2 * i, which).wait_recv()
            across(sp - 2 * i, which).start()

    loads[0].wait()
    near.wait_recv()
    project_kv(pa)
    send_own(pa)
    loads[4].wait()
    project_q(pa)

    fwd = []
    for n in range(CHUNKS):
        far[n].wait_recv()
        ref = x.at[piece(t2, n)]
        cp = remote(ref, ref, fwd_s.at[n], fwd_r.at[n], tp=t1)
        cp.start()
        fwd.append(cp)

    for n in range(CHUNKS):
        fwd[n].wait_recv()
    project_kv(pb)
    send_own(pb)
    relay(pa)
    project_q(pb)

    def attend(src, diagonal):
        kt = jnp.concatenate([kv[src, 0, 0 : HD + extra, :], kv[src, 1, 0 : HD + extra, :]], axis=1)
        vt = jnp.concatenate([kv[src, 0, HD + extra :, :], kv[src, 1, HD + extra :, :]], axis=1)
        for h in range(heads):
            s = lax.dot_general(kt, qt[h], (((0,), (0,)), ((), ())), preferred_element_type=f32)
            lanes = slice(h * HD, (h + 1) * HD)
            if diagonal:
                key_pos = lax.broadcasted_iota(jnp.int32, s.shape, 0)
                query_pos = lax.broadcasted_iota(jnp.int32, s.shape, 1)
                s = jnp.where(key_pos <= query_pos, s, -jnp.inf)
                peak = jnp.max(s, axis=0, keepdims=True)
                w = jnp.exp(s - peak)
                tot[h : h + 1, :] = jnp.sum(w, axis=0, keepdims=True)
                acc[lanes, :] = jnp.dot(vt, w.astype(bf16), preferred_element_type=f32)
            else:
                before = top[h : h + 1, :]
                peak = jnp.maximum(before, jnp.max(s, axis=0, keepdims=True))
                w = jnp.exp(s - peak)
                decay = jnp.exp(before - peak)
                tot[h : h + 1, :] = tot[h : h + 1, :] * decay + jnp.sum(w, axis=0, keepdims=True)
                acc[lanes, :] = acc[lanes, :] * decay + jnp.dot(
                    vt, w.astype(bf16), preferred_element_type=f32
                )
            top[h : h + 1, :] = peak

    attend(sp, True)

    def wait_across(src):
        for which in (pa, pb):
            across(src, which).wait_recv()

    @pl.when(c == 1)
    def _():
        wait_across(spx)
        attend(spx, False)

    relay(pb)

    @pl.loop(1, r + 1)
    def _(i):
        attend(sp - 2 * i, False)

    @pl.loop(1, r + 1)
    def _(i):
        wait_across(spx - 2 * i)
        attend(spx - 2 * i, False)

    for h in range(heads):
        lanes = slice(h * HD, (h + 1) * HD)
        acc[lanes, :] = acc[lanes, :] / tot[h : h + 1, :]
    att[...] = acc[...].T.astype(bf16)
    loads[5].wait()
    width = wo.shape[1] // CHUNKS
    near_sum, far_sum, own_sum = [], [], []
    for n in range(CHUNKS):
        cols = slice(n * width, (n + 1) * width)
        pf[:, cols] = jnp.dot(att[at(pb, half), :], wov[:, cols], preferred_element_type=f32)
        s_near[n] = pf[at(1 - core, rows), cols].astype(bf16)
        cp = remote(s_near.at[n], r_near.at[n], o_s.at[0, n], o_r.at[0, n], tp=t1)
        cp.start()
        near_sum.append(cp)
    for n in range(CHUNKS):
        cols = slice(n * width, (n + 1) * width)
        near_sum[n].wait_recv()
        s_far[n] = (pf[at(core, rows), cols] + r_near[n].astype(f32)).astype(bf16)
        cp = remote(s_far.at[n], r_far.at[n], o_s.at[1, n], o_r.at[1, n], tp=t2)
        cp.start()
        far_sum.append(cp)
    for n in range(CHUNKS):
        cols = slice(n * width, (n + 1) * width)
        own[:, cols] = jnp.dot(att[at(pa, half), :], wov[:, cols], preferred_element_type=f32)
        s_own[n] = own[at(1 - core, rows), cols].astype(bf16)
        cp = remote(s_own.at[n], r_own.at[n], o_s.at[2, n], o_r.at[2, n], tp=t1)
        cp.start()
        own_sum.append(cp)
    for n in range(CHUNKS):
        cols = slice(n * width, (n + 1) * width)
        own_sum[n].wait_recv()
        far_sum[n].wait_recv()
        total = own[at(core, rows), cols] + r_own[n].astype(f32) + r_far[n].astype(f32)
        out[:, cols] = total.astype(bf16)

    near.wait_send()
    for cp in far + fwd + near_sum + far_sum + own_sum:
        cp.wait_send()
    for which in (pa, pb):

        @pl.when(c == 0)
        def _(which=which):
            across(sp, which).wait_send()

        @pl.loop(0, last_row - r)
        def _(i, which=which):
            along(sp, which, last_row - i).wait_send()

        @pl.loop(1, r + 1)
        def _(i, which=which):
            across(sp - 2 * i, which).wait_send()


def per_device(sp_size, tokens, w_query, w_key, w_value, w_out, cum_gate):
    rows, width = tokens.shape
    half, block = 2 * rows, 4 * rows
    heads = w_query.shape[1] // HD
    out_width = w_out.shape[1]
    extra = -(-(3 * heads + 3) // 16) * 16
    bf16, f32 = jnp.bfloat16, jnp.float32
    dma = pltpu.SemaphoreType.DMA
    anywhere = pl.BlockSpec(memory_space=pl.ANY)
    part = pltpu.VMEM((CHUNKS, rows, out_width // CHUNKS), bf16)
    return pl.pallas_call(
        functools.partial(kernel, sp_size),
        out_shape=jax.ShapeDtypeStruct((rows, out_width), bf16),
        in_specs=[anywhere] * 6,
        out_specs=pl.BlockSpec(memory_space=pltpu.VMEM),
        scratch_shapes=[
            pltpu.VMEM((block, width), bf16),
            pltpu.VMEM(w_query.shape, bf16),
            pltpu.VMEM(w_key.shape, bf16),
            pltpu.VMEM(w_value.shape, bf16),
            pltpu.VMEM((width, 2 * HD), bf16),
            pltpu.VMEM(w_out.shape, bf16),
            pltpu.VMEM(cum_gate.shape, f32),
            pltpu.VMEM((sp_size, 2, 2 * HD + extra, half), bf16),
            pltpu.VMEM((heads, HD + extra, block), bf16),
            pltpu.VMEM((heads, block), f32),
            pltpu.VMEM((heads, block), f32),
            pltpu.VMEM((heads * HD, block), f32),
            pltpu.VMEM((block, heads * HD), bf16),
            pltpu.VMEM((half, out_width), f32),
            pltpu.VMEM((half, out_width), f32),
            part, part, part, part, part, part,
            dma((6,)),
            dma((1,)), dma((1,)),
            dma((CHUNKS,)), dma((CHUNKS,)),
            dma((CHUNKS,)), dma((CHUNKS,)),
            dma((sp_size // 2, 2)), dma((sp_size // 2, 2)), dma((sp_size, 2)),
            dma((3, CHUNKS)), dma((3, CHUNKS)),
            pltpu.SemaphoreType.REGULAR,
        ],
        compiler_params=pltpu.CompilerParams(
            collective_id=0, has_side_effects=True, vmem_limit_bytes=48 * 1024 * 1024
        ),
    )(tokens, w_query, w_key, w_value, w_out, cum_gate)


def solution(mesh):
    placed = (
        P(("sp", "tp"), None),
        P(None, "tp"),
        P(None, "tp"),
        P(None, "tp"),
        P("tp", None),
        P("tp", "sp"),
    )
    return jax.shard_map(
        functools.partial(per_device, mesh.shape["sp"]),
        mesh=mesh, in_specs=placed, out_specs=P(("sp", "tp"), None), check_vma=False,
    )
```

```python
import functools

import jax
import jax.numpy as jnp
from jax import lax
from jax.experimental import pallas as pl
from jax.experimental.pallas import tpu as pltpu
from jax.sharding import PartitionSpec as P

HD = 64
MESH = pl.DeviceIdType.MESH
CHUNKS = 4


def kernel(
    sp_size, tok, wq, wk, wv, wo, gate, out,
    x, wqv, wboth, wov, gv, kv, qt, top, tot, acc, att, pf, own,
    s_near, s_far, s_own, r_near, r_far, r_own,
    load, tok_s, tok_r, far_s, far_r, fwd_s, fwd_r,
    z_s, x_s, kv_r, o_s, o_r, ready,
):
    f32, bf16 = jnp.float32, jnp.bfloat16
    rows = tok.shape[0]
    half = 2 * rows
    block = 2 * half
    heads = wq.shape[1] // HD
    sp = lax.axis_index("sp")
    t = lax.axis_index("tp")
    core = lax.rem(t, 2)
    p = t // 2
    t1 = t + 1 - 2 * core
    t2 = lax.rem(t + 2, 4)
    r = sp // 2
    c = lax.rem(sp, 2)
    last_row = sp_size // 2 - 1
    spx = sp + 1 - 2 * c
    has_next = r < last_row
    pa, pb = p, 1 - p

    def at(n, unit):
        return pl.ds(pl.multiple_of(n * unit, unit), unit)

    loads = [
        pltpu.make_async_copy(tok, x.at[at(t, rows)], load.at[0]),
        pltpu.make_async_copy(gate, gv, load.at[1]),
        pltpu.make_async_copy(wk, wboth.at[0:HD], load.at[2]),
        pltpu.make_async_copy(wv, wboth.at[HD : 2 * HD], load.at[3]),
        pltpu.make_async_copy(wq, wqv, load.at[4]),
        pltpu.make_async_copy(wo, wov, load.at[5]),
    ]
    for copy in loads:
        copy.start()

    barrier = pltpu.get_barrier_semaphore()
    pl.semaphore_signal(barrier, inc=1, device_id={"tp": t1}, device_id_type=MESH)
    pl.semaphore_signal(barrier, inc=1, device_id={"tp": t2}, device_id_type=MESH)
    pl.semaphore_signal(barrier, inc=1, device_id={"sp": spx}, device_id_type=MESH)

    @pl.when(has_next)
    def _():
        pl.semaphore_signal(barrier, inc=1, device_id={"sp": sp + 2}, device_id_type=MESH)

    @pl.when(r > 0)
    def _():
        pl.semaphore_signal(barrier, inc=1, device_id={"sp": sp - 2}, device_id_type=MESH)

    peers = 3 + jnp.where(has_next, 1, 0) + jnp.where(r > 0, 1, 0)
    pl.semaphore_wait(barrier, peers)

    step = rows // CHUNKS

    def piece(shard, n):
        return pl.ds(pl.multiple_of(shard * rows + n * step, step), step)

    def remote(src, dst, ss, rs, **where):
        return pltpu.make_async_remote_copy(
            src_ref=src, dst_ref=dst, send_sem=ss, recv_sem=rs,
            device_id=where, device_id_type=MESH,
        )

    far = []
    for n in range(CHUNKS):
        cp = remote(tok.at[pl.ds(n * step, step)], x.at[piece(t, n)], far_s.at[n], far_r.at[n], tp=t2)
        cp.start()
        far.append(cp)
    near = remote(tok, x.at[at(t, rows)], tok_s.at[0], tok_r.at[0], tp=t1)
    near.start()

    loads[1].wait()
    g = gv[...]
    hi = g.astype(bf16).astype(f32)
    mid = (g - hi).astype(bf16).astype(f32)
    low = (g - hi - mid).astype(bf16).astype(f32)
    parts = (hi, mid, low)
    extra = kv.shape[2] - 2 * HD
    index = lax.broadcasted_iota(jnp.int32, (extra, block), 0)
    key_side = jnp.where((index >= 3 * heads) & (index < 3 * heads + 3), 1.0, 0.0).astype(f32)
    for k in range(3):
        for h in range(heads):
            key_side = jnp.where(index == k * heads + h, -parts[k][h : h + 1, :], key_side)
    key_side = key_side.astype(bf16)
    kv[sp, 0, HD : HD + extra, :] = key_side[:, :half]
    kv[sp, 1, HD : HD + extra, :] = key_side[:, half:]
    for h in range(heads):
        side = jnp.where((index < 3 * heads) & (lax.rem(index, heads) == h), 1.0, 0.0).astype(f32)
        for k in range(3):
            side = jnp.where(index == 3 * heads + k, parts[k][h : h + 1, :], side)
        qt[h, HD : HD + extra, :] = side.astype(bf16)

    def project_kv(which):
        xs = x[at(which, half), :]
        both = lax.dot_general(
            wboth[...], xs, (((1,), (1,)), ((), ())), preferred_element_type=f32
        ).astype(bf16)
        kv[sp, which, 0:HD, :] = both[:HD]
        kv[sp, which, HD + extra :, :] = both[HD:]

    def project_q(which):
        xs = x[at(which, half), :]
        q = jnp.dot(xs, wqv[...], preferred_element_type=f32).astype(bf16).astype(f32)
        q = (q * (float(HD) ** -0.5)).T.astype(bf16)
        for h in range(heads):
            qt[h, 0:HD, at(which, half)] = q[h * HD : (h + 1) * HD]

    def along(src, which, row):
        ref = kv.at[src, which]
        return remote(ref, ref, z_s.at[row, which], kv_r.at[src, which], sp=2 * row + c)

    def across(src, which):
        ref = kv.at[src, which]
        return remote(ref, ref, x_s.at[src // 2, which], kv_r.at[src, which], sp=spx)

    def send_own(which):
        @pl.loop(0, last_row - r)
        def _(i):
            along(sp, which, last_row - i).start()

        @pl.when(c == 0)
        def _():
            across(sp, which).start()

    def relay(which):
        @pl.loop(1, r + 1)
        def _(i):
            across(sp - 2 * i, which).wait_recv()
            across(sp - 2 * i, which).start()

    def hear():
        @pl.when(r < last_row - 1)
        def _():
            pl.semaphore_wait(ready, 1)

    @pl.when(r > 0)
    def _():
        hear()

        @pl.when(has_next)
        def _():
            pl.semaphore_signal(ready, inc=1, device_id={"sp": sp - 2}, device_id_type=MESH)

    loads[0].wait()
    loads[2].wait()
    loads[3].wait()
    near.wait_recv()
    project_kv(pa)

    @pl.when(r == 0)
    def _():
        hear()

    send_own(pa)
    loads[4].wait()
    project_q(pa)

    fwd = []
    for n in range(CHUNKS):
        far[n].wait_recv()
        ref = x.at[piece(t2, n)]
        cp = remote(ref, ref, fwd_s.at[n], fwd_r.at[n], tp=t1)
        cp.start()
        fwd.append(cp)

    for n in range(CHUNKS):
        fwd[n].wait_recv()
    project_kv(pb)
    send_own(pb)
    relay(pa)
    project_q(pb)

    def attend(src, diagonal):
        kt = jnp.concatenate([kv[src, 0, 0 : HD + extra, :], kv[src, 1, 0 : HD + extra, :]], axis=1)
        vt = jnp.concatenate([kv[src, 0, HD + extra :, :], kv[src, 1, HD + extra :, :]], axis=1)
        for h in range(heads):
            s = lax.dot_general(kt, qt[h], (((0,), (0,)), ((), ())), preferred_element_type=f32)
            lanes = slice(h * HD, (h + 1) * HD)
            if diagonal:
                key_pos = lax.broadcasted_iota(jnp.int32, s.shape, 0)
                query_pos = lax.broadcasted_iota(jnp.int32, s.shape, 1)
                s = jnp.where(key_pos <= query_pos, s, -jnp.inf)
                peak = jnp.max(s, axis=0, keepdims=True)
                w = jnp.exp(s - peak)
                tot[h : h + 1, :] = jnp.sum(w, axis=0, keepdims=True)
                acc[lanes, :] = jnp.dot(vt, w.astype(bf16), preferred_element_type=f32)
            else:
                before = top[h : h + 1, :]
                peak = jnp.maximum(before, jnp.max(s, axis=0, keepdims=True))
                w = jnp.exp(s - peak)
                decay = jnp.exp(before - peak)
                tot[h : h + 1, :] = tot[h : h + 1, :] * decay + jnp.sum(w, axis=0, keepdims=True)
                acc[lanes, :] = acc[lanes, :] * decay + jnp.dot(
                    vt, w.astype(bf16), preferred_element_type=f32
                )
            top[h : h + 1, :] = peak

    attend(sp, True)

    def wait_across(src):
        for which in (pa, pb):
            across(src, which).wait_recv()

    @pl.when(c == 1)
    def _():
        wait_across(spx)
        attend(spx, False)

    relay(pb)

    @pl.loop(1, r + 1)
    def _(i):
        attend(sp - 2 * i, False)

    @pl.loop(1, r + 1)
    def _(i):
        wait_across(spx - 2 * i)
        attend(spx - 2 * i, False)

    for h in range(heads):
        lanes = slice(h * HD, (h + 1) * HD)
        acc[lanes, :] = acc[lanes, :] / tot[h : h + 1, :]
    att[...] = acc[...].T.astype(bf16)
    loads[5].wait()
    width = wo.shape[1] // CHUNKS
    near_sum, far_sum, own_sum = [], [], []
    for n in range(CHUNKS):
        cols = slice(n * width, (n + 1) * width)
        pf[:, cols] = jnp.dot(att[at(pb, half), :], wov[:, cols], preferred_element_type=f32)
        s_near[n] = pf[at(1 - core, rows), cols].astype(bf16)
        cp = remote(s_near.at[n], r_near.at[n], o_s.at[0, n], o_r.at[0, n], tp=t1)
        cp.start()
        near_sum.append(cp)
    for n in range(CHUNKS):
        cols = slice(n * width, (n + 1) * width)
        near_sum[n].wait_recv()
        s_far[n] = (pf[at(core, rows), cols] + r_near[n].astype(f32)).astype(bf16)
        cp = remote(s_far.at[n], r_far.at[n], o_s.at[1, n], o_r.at[1, n], tp=t2)
        cp.start()
        far_sum.append(cp)
    for n in range(CHUNKS):
        cols = slice(n * width, (n + 1) * width)
        own[:, cols] = jnp.dot(att[at(pa, half), :], wov[:, cols], preferred_element_type=f32)
        s_own[n] = own[at(1 - core, rows), cols].astype(bf16)
        cp = remote(s_own.at[n], r_own.at[n], o_s.at[2, n], o_r.at[2, n], tp=t1)
        cp.start()
        own_sum.append(cp)
    for n in range(CHUNKS):
        cols = slice(n * width, (n + 1) * width)
        own_sum[n].wait_recv()
        far_sum[n].wait_recv()
        total = own[at(core, rows), cols] + r_own[n].astype(f32) + r_far[n].astype(f32)
        out[:, cols] = total.astype(bf16)

    near.wait_send()
    for cp in far + fwd + near_sum + far_sum + own_sum:
        cp.wait_send()
    for which in (pa, pb):

        @pl.when(c == 0)
        def _(which=which):
            across(sp, which).wait_send()

        @pl.loop(0, last_row - r)
        def _(i, which=which):
            along(sp, which, last_row - i).wait_send()

        @pl.loop(1, r + 1)
        def _(i, which=which):
            across(sp - 2 * i, which).wait_send()


def per_device(sp_size, tokens, w_query, w_key, w_value, w_out, cum_gate):
    rows, width = tokens.shape
    half, block = 2 * rows, 4 * rows
    heads = w_query.shape[1] // HD
    out_width = w_out.shape[1]
    extra = -(-(3 * heads + 3) // 16) * 16
    bf16, f32 = jnp.bfloat16, jnp.float32
    dma = pltpu.SemaphoreType.DMA
    anywhere = pl.BlockSpec(memory_space=pl.ANY)
    part = pltpu.VMEM((CHUNKS, rows, out_width // CHUNKS), bf16)
    return pl.pallas_call(
        functools.partial(kernel, sp_size),
        out_shape=jax.ShapeDtypeStruct((rows, out_width), bf16),
        in_specs=[anywhere] * 6,
        out_specs=pl.BlockSpec(memory_space=pltpu.VMEM),
        scratch_shapes=[
            pltpu.VMEM((block, width), bf16),
            pltpu.VMEM(w_query.shape, bf16),
            pltpu.VMEM((2 * HD, width), bf16),
            pltpu.VMEM(w_out.shape, bf16),
            pltpu.VMEM(cum_gate.shape, f32),
            pltpu.VMEM((sp_size, 2, 2 * HD + extra, half), bf16),
            pltpu.VMEM((heads, HD + extra, block), bf16),
            pltpu.VMEM((heads, block), f32),
            pltpu.VMEM((heads, block), f32),
            pltpu.VMEM((heads * HD, block), f32),
            pltpu.VMEM((block, heads * HD), bf16),
            pltpu.VMEM((half, out_width), f32),
            pltpu.VMEM((half, out_width), f32),
            part, part, part, part, part, part,
            dma((6,)),
            dma((1,)), dma((1,)),
            dma((CHUNKS,)), dma((CHUNKS,)),
            dma((CHUNKS,)), dma((CHUNKS,)),
            dma((sp_size // 2, 2)), dma((sp_size // 2, 2)), dma((sp_size, 2)),
            dma((3, CHUNKS)), dma((3, CHUNKS)),
            pltpu.SemaphoreType.REGULAR,
        ],
        compiler_params=pltpu.CompilerParams(
            collective_id=0, has_side_effects=True, vmem_limit_bytes=62 * 1024 * 1024
        ),
    )(tokens, w_query, w_key.T, w_value.T, w_out, cum_gate)


def solution(mesh):
    placed = (
        P(("sp", "tp"), None),
        P(None, "tp"),
        P(None, "tp"),
        P(None, "tp"),
        P("tp", None),
        P("tp", "sp"),
    )
    return jax.shard_map(
        functools.partial(per_device, mesh.shape["sp"]),
        mesh=mesh, in_specs=placed, out_specs=P(("sp", "tp"), None), check_vma=False,
    )
```

```python
import functools

import jax
import jax.numpy as jnp
from jax import lax
from jax.experimental import pallas as pl
from jax.experimental.pallas import tpu as pltpu
from jax.sharding import PartitionSpec as P

HD = 64
MESH = pl.DeviceIdType.MESH
CHUNKS = 4


def kernel(
    sp_size, tok, wq, wk, wv, wo, gate, out,
    x, wqv, wboth, wov, gv, kv, qt, top, tot, acc, att, pf, own,
    s_near, s_far, s_own, r_near, r_far, r_own,
    load, tok_s, tok_r, far_s, far_r, fwd_s, fwd_r,
    z_s, x_s, kv_r, o_s, o_r, ready,
    wg, ag, w_s, w_r, a_s, a_r,
):
    f32, bf16 = jnp.float32, jnp.bfloat16
    rows = tok.shape[0]
    half = 2 * rows
    block = 2 * half
    heads = wq.shape[1] // HD
    sp = lax.axis_index("sp")
    t = lax.axis_index("tp")
    core = lax.rem(t, 2)
    p = t // 2
    t1 = t + 1 - 2 * core
    t2 = lax.rem(t + 2, 4)
    t3 = 3 - t
    r = sp // 2
    c = lax.rem(sp, 2)
    last_row = sp_size // 2 - 1
    spx = sp + 1 - 2 * c
    has_next = r < last_row
    pa, pb = p, 1 - p

    def at(n, unit):
        return pl.ds(pl.multiple_of(n * unit, unit), unit)

    loads = [
        pltpu.make_async_copy(tok, x.at[at(t, rows)], load.at[0]),
        pltpu.make_async_copy(gate, gv, load.at[1]),
        pltpu.make_async_copy(wk, wboth.at[0:HD], load.at[2]),
        pltpu.make_async_copy(wv, wboth.at[HD : 2 * HD], load.at[3]),
        pltpu.make_async_copy(wq, wqv, load.at[4]),
        pltpu.make_async_copy(wo, wov, load.at[5]),
    ]
    for copy in loads:
        copy.start()

    barrier = pltpu.get_barrier_semaphore()
    pl.semaphore_signal(barrier, inc=1, device_id={"tp": t1}, device_id_type=MESH)
    pl.semaphore_signal(barrier, inc=1, device_id={"tp": t2}, device_id_type=MESH)
    pl.semaphore_signal(barrier, inc=1, device_id={"tp": t3}, device_id_type=MESH)
    pl.semaphore_signal(barrier, inc=1, device_id={"sp": spx}, device_id_type=MESH)

    @pl.when(has_next)
    def _():
        pl.semaphore_signal(barrier, inc=1, device_id={"sp": sp + 2}, device_id_type=MESH)

    @pl.when(r > 0)
    def _():
        pl.semaphore_signal(barrier, inc=1, device_id={"sp": sp - 2}, device_id_type=MESH)

    peers = 4 + jnp.where(has_next, 1, 0) + jnp.where(r > 0, 1, 0)
    pl.semaphore_wait(barrier, peers)

    step = rows // CHUNKS

    def piece(shard, n):
        return pl.ds(pl.multiple_of(shard * rows + n * step, step), step)

    def remote(src, dst, ss, rs, **where):
        return pltpu.make_async_remote_copy(
            src_ref=src, dst_ref=dst, send_sem=ss, recv_sem=rs,
            device_id=where, device_id_type=MESH,
        )

    far = []
    for n in range(CHUNKS):
        cp = remote(tok.at[pl.ds(n * step, step)], x.at[piece(t, n)], far_s.at[n], far_r.at[n], tp=t2)
        cp.start()
        far.append(cp)
    near = remote(tok, x.at[at(t, rows)], tok_s.at[0], tok_r.at[0], tp=t1)
    near.start()

    loads[1].wait()
    g = gv[...]
    hi = g.astype(bf16).astype(f32)
    mid = (g - hi).astype(bf16).astype(f32)
    low = (g - hi - mid).astype(bf16).astype(f32)
    parts = (hi, mid, low)
    extra = kv.shape[2] - 2 * HD
    index = lax.broadcasted_iota(jnp.int32, (extra, block), 0)
    key_side = jnp.where((index >= 3 * heads) & (index < 3 * heads + 3), 1.0, 0.0).astype(f32)
    for k in range(3):
        for h in range(heads):
            key_side = jnp.where(index == k * heads + h, -parts[k][h : h + 1, :], key_side)
    key_side = key_side.astype(bf16)
    kv[sp, 0, HD : HD + extra, :] = key_side[:, :half]
    kv[sp, 1, HD : HD + extra, :] = key_side[:, half:]
    for h in range(heads):
        side = jnp.where((index < 3 * heads) & (lax.rem(index, heads) == h), 1.0, 0.0).astype(f32)
        for k in range(3):
            side = jnp.where(index == 3 * heads + k, parts[k][h : h + 1, :], side)
        qt[h, HD : HD + extra, :] = side.astype(bf16)

    def project_kv(which):
        xs = x[at(which, half), :]
        both = lax.dot_general(
            wboth[...], xs, (((1,), (1,)), ((), ())), preferred_element_type=f32
        ).astype(bf16)
        kv[sp, which, 0:HD, :] = both[:HD]
        kv[sp, which, HD + extra :, :] = both[HD:]

    def project_q(which):
        xs = x[at(which, half), :]
        q = jnp.dot(xs, wqv[...], preferred_element_type=f32).astype(bf16).astype(f32)
        q = (q * (float(HD) ** -0.5)).T.astype(bf16)
        for h in range(heads):
            qt[h, 0:HD, at(which, half)] = q[h * HD : (h + 1) * HD]

    def along(src, which, row):
        ref = kv.at[src, which]
        return remote(ref, ref, z_s.at[row, which], kv_r.at[src, which], sp=2 * row + c)

    def across(src, which):
        ref = kv.at[src, which]
        return remote(ref, ref, x_s.at[src // 2, which], kv_r.at[src, which], sp=spx)

    def send_own(which):
        @pl.loop(0, last_row - r)
        def _(i):
            along(sp, which, last_row - i).start()

        @pl.when(c == 0)
        def _():
            across(sp, which).start()

    def relay(which):
        @pl.loop(1, r + 1)
        def _(i):
            across(sp - 2 * i, which).wait_recv()
            across(sp - 2 * i, which).start()

    def hear():
        @pl.when(r < last_row - 1)
        def _():
            pl.semaphore_wait(ready, 1)

    @pl.when(r > 0)
    def _():
        hear()

        @pl.when(has_next)
        def _():
            pl.semaphore_signal(ready, inc=1, device_id={"sp": sp - 2}, device_id_type=MESH)

    loads[0].wait()
    loads[2].wait()
    loads[3].wait()
    near.wait_recv()
    project_kv(pa)

    @pl.when(r == 0)
    def _():
        hear()

    send_own(pa)
    loads[4].wait()
    project_q(pa)

    fwd = []
    for n in range(CHUNKS):
        far[n].wait_recv()
        ref = x.at[piece(t2, n)]
        cp = remote(ref, ref, fwd_s.at[n], fwd_r.at[n], tp=t1)
        cp.start()
        fwd.append(cp)

    loads[5].wait()
    split = wo.shape[1] // 2
    gathered = pl.ds(0, split)
    w_far = remote(wov.at[:, gathered], wg.at[t], w_s.at[1], w_r.at[1], tp=t2)
    w_near = remote(wov.at[:, gathered], wg.at[t], w_s.at[0], w_r.at[0], tp=t1)
    w_far.start()

    for n in range(CHUNKS):
        fwd[n].wait_recv()
    w_near.start()
    project_kv(pb)
    send_own(pb)
    relay(pa)
    project_q(pb)

    def attend(src, diagonal):
        kt = jnp.concatenate([kv[src, 0, 0 : HD + extra, :], kv[src, 1, 0 : HD + extra, :]], axis=1)
        vt = jnp.concatenate([kv[src, 0, HD + extra :, :], kv[src, 1, HD + extra :, :]], axis=1)
        for h in range(heads):
            s = lax.dot_general(kt, qt[h], (((0,), (0,)), ((), ())), preferred_element_type=f32)
            lanes = slice(h * HD, (h + 1) * HD)
            if diagonal:
                key_pos = lax.broadcasted_iota(jnp.int32, s.shape, 0)
                query_pos = lax.broadcasted_iota(jnp.int32, s.shape, 1)
                s = jnp.where(key_pos <= query_pos, s, -jnp.inf)
                peak = jnp.max(s, axis=0, keepdims=True)
                w = jnp.exp(s - peak)
                tot[h : h + 1, :] = jnp.sum(w, axis=0, keepdims=True)
                acc[lanes, :] = jnp.dot(vt, w.astype(bf16), preferred_element_type=f32)
            else:
                before = top[h : h + 1, :]
                peak = jnp.maximum(before, jnp.max(s, axis=0, keepdims=True))
                w = jnp.exp(s - peak)
                decay = jnp.exp(before - peak)
                tot[h : h + 1, :] = tot[h : h + 1, :] * decay + jnp.sum(w, axis=0, keepdims=True)
                acc[lanes, :] = acc[lanes, :] * decay + jnp.dot(
                    vt, w.astype(bf16), preferred_element_type=f32
                )
            top[h : h + 1, :] = peak

    attend(sp, True)

    def wait_across(src):
        for which in (pa, pb):
            across(src, which).wait_recv()

    @pl.when(c == 1)
    def _():
        wait_across(spx)
        attend(spx, False)

    relay(pb)

    @pl.loop(1, r + 1)
    def _(i):
        attend(sp - 2 * i, False)

    @pl.loop(1, r + 1)
    def _(i):
        wait_across(spx - 2 * i)
        attend(spx - 2 * i, False)

    for h in range(heads):
        lanes = slice(h * HD, (h + 1) * HD)
        acc[lanes, :] = acc[lanes, :] / tot[h : h + 1, :]
    att[...] = acc[...].T.astype(bf16)
    exchange = []
    for n, peer in ((1, t2), (2, t3), (0, t1)):
        cp = remote(att.at[at(peer, rows)], ag.at[t], a_s.at[n], a_r.at[n], tp=peer)
        cp.start()
        exchange.append(cp)
    width = (wo.shape[1] - split) // CHUNKS
    near_sum, far_sum, own_sum = [], [], []
    for n in range(CHUNKS):
        cols = slice(split + n * width, split + (n + 1) * width)
        pf[:, cols] = jnp.dot(att[at(pb, half), :], wov[:, cols], preferred_element_type=f32)
        s_near[n] = pf[at(1 - core, rows), cols].astype(bf16)
        cp = remote(s_near.at[n], r_near.at[n], o_s.at[0, n], o_r.at[0, n], tp=t1)
        cp.start()
        near_sum.append(cp)
    for n in range(CHUNKS):
        cols = slice(split + n * width, split + (n + 1) * width)
        near_sum[n].wait_recv()
        s_far[n] = (pf[at(core, rows), cols] + r_near[n].astype(f32)).astype(bf16)
        cp = remote(s_far.at[n], r_far.at[n], o_s.at[1, n], o_r.at[1, n], tp=t2)
        cp.start()
        far_sum.append(cp)
    for n in range(CHUNKS):
        cols = slice(split + n * width, split + (n + 1) * width)
        own[:, cols] = jnp.dot(att[at(pa, half), :], wov[:, cols], preferred_element_type=f32)
        s_own[n] = own[at(1 - core, rows), cols].astype(bf16)
        cp = remote(s_own.at[n], r_own.at[n], o_s.at[2, n], o_r.at[2, n], tp=t1)
        cp.start()
        own_sum.append(cp)

    w_far.wait_recv()
    w_fwd = remote(wg.at[t2], wg.at[t2], w_s.at[2], w_r.at[2], tp=t1)
    w_fwd.start()
    total = jnp.dot(att[at(t, rows), :], wov[:, gathered], preferred_element_type=f32)
    for waits, peer in (((w_near, exchange[2]), t1), ((exchange[0],), t2), ((w_fwd, exchange[1]), t3)):
        for cp in waits:
            cp.wait_recv()
        total = total + jnp.dot(ag[peer], wg[peer], preferred_element_type=f32)
    out[:, gathered] = total.astype(bf16)
    for n in range(CHUNKS):
        cols = slice(split + n * width, split + (n + 1) * width)
        own_sum[n].wait_recv()
        far_sum[n].wait_recv()
        total = own[at(core, rows), cols] + r_own[n].astype(f32) + r_far[n].astype(f32)
        out[:, cols] = total.astype(bf16)

    near.wait_send()
    for cp in far + fwd + near_sum + far_sum + own_sum + exchange + [w_far, w_near, w_fwd]:
        cp.wait_send()
    for which in (pa, pb):

        @pl.when(c == 0)
        def _(which=which):
            across(sp, which).wait_send()

        @pl.loop(0, last_row - r)
        def _(i, which=which):
            along(sp, which, last_row - i).wait_send()

        @pl.loop(1, r + 1)
        def _(i, which=which):
            across(sp - 2 * i, which).wait_send()


def per_device(sp_size, tokens, w_query, w_key, w_value, w_out, cum_gate):
    rows, width = tokens.shape
    half, block = 2 * rows, 4 * rows
    heads = w_query.shape[1] // HD
    out_width = w_out.shape[1]
    extra = -(-(3 * heads + 3) // 16) * 16
    bf16, f32 = jnp.bfloat16, jnp.float32
    dma = pltpu.SemaphoreType.DMA
    anywhere = pl.BlockSpec(memory_space=pl.ANY)
    part = pltpu.VMEM((CHUNKS, rows, out_width // 2 // CHUNKS), bf16)
    return pl.pallas_call(
        functools.partial(kernel, sp_size),
        out_shape=jax.ShapeDtypeStruct((rows, out_width), bf16),
        in_specs=[anywhere] * 6,
        out_specs=pl.BlockSpec(memory_space=pltpu.VMEM),
        scratch_shapes=[
            pltpu.VMEM((block, width), bf16),
            pltpu.VMEM(w_query.shape, bf16),
            pltpu.VMEM((2 * HD, width), bf16),
            pltpu.VMEM(w_out.shape, bf16),
            pltpu.VMEM(cum_gate.shape, f32),
            pltpu.VMEM((sp_size, 2, 2 * HD + extra, half), bf16),
            pltpu.VMEM((heads, HD + extra, block), bf16),
            pltpu.VMEM((heads, block), f32),
            pltpu.VMEM((heads, block), f32),
            pltpu.VMEM((heads * HD, block), f32),
            pltpu.VMEM((block, heads * HD), bf16),
            pltpu.VMEM((half, out_width), f32),
            pltpu.VMEM((half, out_width), f32),
            part, part, part, part, part, part,
            dma((6,)),
            dma((1,)), dma((1,)),
            dma((CHUNKS,)), dma((CHUNKS,)),
            dma((CHUNKS,)), dma((CHUNKS,)),
            dma((sp_size // 2, 2)), dma((sp_size // 2, 2)), dma((sp_size, 2)),
            dma((3, CHUNKS)), dma((3, CHUNKS)),
            pltpu.SemaphoreType.REGULAR,
            pltpu.VMEM((4, w_out.shape[0], out_width // 2), bf16),
            pltpu.VMEM((4, rows, w_out.shape[0]), bf16),
            dma((3,)), dma((3,)), dma((3,)), dma((3,)),
        ],
        compiler_params=pltpu.CompilerParams(
            collective_id=0, has_side_effects=True, vmem_limit_bytes=62 * 1024 * 1024
        ),
    )(tokens, w_query, w_key.T, w_value.T, w_out, cum_gate)


def solution(mesh):
    placed = (
        P(("sp", "tp"), None),
        P(None, "tp"),
        P(None, "tp"),
        P(None, "tp"),
        P("tp", None),
        P("tp", "sp"),
    )
    return jax.shard_map(
        functools.partial(per_device, mesh.shape["sp"]),
        mesh=mesh, in_specs=placed, out_specs=P(("sp", "tp"), None), check_vma=False,
    )
```
